32 devices in a mesh: fs: 4 (over z), rep: 4 (over y, x), tp: 2 (over core).
Axes of the slice: x: 2, y: 2, z: 4, core: 2. Of those that a mesh axis runs over, the one named last changes fastest.
Arguments:
- mixer_out: bfloat16 [16384, 1536], P(('fs', 'rep')), may hold values from -6 to 6
- out_grad: bfloat16 [16384, 4096], P(('fs', 'rep'), 'tp'), may hold values from -0.046875 to 0.046875
- factors: bfloat16 [1536, 256], P(('fs', 'rep')), may hold values from -0.15625 to 0.15625
- weight: float32 [1536, 4096], P(('fs', 'rep'), 'tp'), may hold values from -0.15625 to 0.15625
- first_moment: float32 [256, 4096], P(('fs', 'rep'), 'tp'), may hold values from -6 to 6
- second_moment: float32 [256, 4096], P(('fs', 'rep'), 'tp'), may hold values from 0.05 to 2
Outputs:
- new_weight: float32 [1536, 4096], P(('fs', 'rep'), 'tp')
- update: float32 [1536, 4096], P(('fs', 'rep'), 'tp')
- new_first: float32 [256, 4096], P(('fs', 'rep'), 'tp')
- new_second: float32 [256, 4096], P(('fs', 'rep'), 'tp')
- weight_copy: bfloat16 [1536, 4096], P(None, 'tp')
The draws below stay inside these ranges and needn't reach their ends.
All inputs are finite; a program needn't handle non-finite values.
Results may differ from the reference program's by a relative error of at most 0.0034.
Values may be sent and summed in bfloat16 or wider, within the bound.
No kernel may reach another device: no remote copies, remote signals or barrier semaphores. Data moves between devices by JAX's collectives and lax.ppermute only.
A program may use at most 64 MiB of HBM per device.

```python
import math
import jax
import jax.numpy as jnp

D = 4096
DH = 1536
RANK = 256
TOK_DEV = 1024
TOKENS = 16384
N_FS = 4
N_REP = 4


def raised(result, rng, source, target, shards_of, factor):
    owner, partner = [(jnp.arange(result.shape[dim]) // (result.shape[dim] // shards_of)).reshape([-1 if axis == dim else 1 for axis in range(result.ndim)]) for dim in (source, target)]
    chosen = jax.random.permutation(rng, shards_of)[partner]
    strong = (owner == chosen) | (owner == (partner + shards_of // 2) % shards_of)
    return jnp.where(strong, factor * result, result)


def block_levels(own_key, dims, cuts, smallest, high):
    def one(axis_at, blocks):
        draws = jax.random.uniform(jax.random.fold_in(jax.random.fold_in(own_key, 6), axis_at), (blocks,), jnp.float32, smallest / len(cuts), high / len(cuts))
        return jnp.repeat(jnp.exp(draws), dims[axis_at] // blocks).reshape((-1,) + (1,) * (len(dims) - axis_at - 1))

    level = one(*cuts[0])
    for cut in cuts[1:]:
        level = level * one(*cut)
    return level


def noise(own_key, dims, scale, limit, pieces=(), dtype=jnp.bfloat16):
    drawn = jax.random.normal(own_key, dims, jnp.float32) * scale
    if len(pieces) > 0:
        drawn = block_levels(own_key, dims, pieces, -0.22, 0.18) * drawn
    return jnp.clip(drawn, min=-limit, max=limit).astype(dtype)


def bell_draw_with(stream_key, dims, spread, most, pieces, heavy, kind=jnp.bfloat16):
    entries = spread * jax.random.normal(stream_key, dims, jnp.float32)
    if pieces:
        entries = entries * block_levels(stream_key, dims, pieces, -0.22, 0.18)
    return jnp.clip(raised(entries, jax.random.fold_in(stream_key, 3), *heavy), -most, most).astype(kind)


def setup_inputs(seed: int = 0) -> dict:
    arg_keys = jax.random.split(jax.random.key(seed), 7)
    return {
        "mixer_out": bell_draw_with(arg_keys[0], (TOKENS, DH), 1.0, 6.0, ((0, 16),), (0, 1, 16, 2.0)),
        "out_grad": noise(arg_keys[1], (TOKENS, D), ((TOK_DEV * N_FS * N_REP) ** -0.5), 0.046875, ((0, 16), (1, 2))),
        "factors": noise(arg_keys[2], (DH, RANK), DH ** -0.5, 0.15625, ((0, 16),)),
        "weight": noise(arg_keys[3], (DH, D), DH ** -0.5, 0.15625, ((0, 16), (1, 2)), jnp.float32),
        "first_moment": noise(arg_keys[4], (RANK, D), 1.0, 6.0, ((0, 16), (1, 2)), jnp.float32),
        "second_moment": jnp.clip(jnp.exp(math.log(2.0) - 3.6888794 * jax.random.uniform(arg_keys[5], (RANK, D), jnp.float32) ** block_levels(arg_keys[5], (RANK, D), ((0, 16), (1, 2)), -0.2, 0.2)), 0.05, 2.0),
    }


def reference(mixer_out, out_grad, factors, weight, first_moment, second_moment):
    gradient = jnp.dot(mixer_out.T, out_grad, preferred_element_type=jnp.float32)
    grad_low = gradient.astype(jnp.bfloat16)
    projected = jnp.dot(factors.T, grad_low, preferred_element_type=jnp.float32)
    new_first = 0.8 * first_moment + 0.2 * projected
    new_second = 0.9 * second_moment + 0.1 * projected * projected
    direction = new_first / (jnp.sqrt(new_second) + 1e-08)
    dir_low = direction.astype(jnp.bfloat16)
    proj_low = projected.astype(jnp.bfloat16)
    dir_wide = dir_low.astype(jnp.float32)
    proj_wide = proj_low.astype(jnp.float32)
    scale_ratio = jnp.sqrt(jnp.sum(dir_wide * dir_wide)) / jnp.sqrt(jnp.sum(proj_wide * proj_wide) + 1e-06)
    back_dir = jnp.dot(factors, dir_low, preferred_element_type=jnp.float32)
    back_proj = jnp.dot(factors, proj_low, preferred_element_type=jnp.float32)
    update = back_dir + scale_ratio * (gradient - back_proj)
    new_weight = weight - 0.01 * update
    weight_copy = new_weight.astype(jnp.bfloat16)
    return (new_weight, update, new_first, new_second, weight_copy)
```

```python
import functools

import jax
import jax.numpy as jnp
from jax import lax
from jax.experimental import pallas as pl
from jax.experimental.pallas import tpu as pltpu
from jax.sharding import PartitionSpec as P


BF = jnp.bfloat16
F32 = jnp.float32


def gray(z):
    return z ^ (z >> 1)


def ungray(h, n):
    z, step = h, 1
    while step < n:
        z = z ^ (z >> step)
        step *= 2
    return z


def bits_of(n):
    return [1 << k for k in range(n.bit_length() - 1)]


def swap(a, axis, bit, n):
    if axis == "fs":
        pairs = [(z, ungray(gray(z) ^ bit, n)) for z in range(n)]
    else:
        pairs = [(i, i ^ bit) for i in range(n)]
    return lax.ppermute(a, axis, pairs)


def grad_kernel(send_a, send_b, R, zs, reps, m, oa, ob, *refs):
    acc = refs[-1]
    ns = 2
    outs = refs[:-1]
    sends, keeps = outs[:ns], list(outs[ns:])
    nr = reps.shape[0]
    for send, out, o in ((send_a, sends[0], oa), (send_b, sends[1], ob)):
        acc[...] = lax.dot_general(
            m[...].reshape(m.shape[-2:]), o[...], (((0,), (0,)), ((), ())), preferred_element_type=F32
        )
        for rel in range(nr):
            rows = acc[pl.ds(pl.multiple_of(reps[rel] * R, 8), R), :]
            if rel in send:
                out[0, send.index(rel)] = rows.astype(BF)
            else:
                keeps.pop(0)[0] = rows


def grad_blocks(mixer_out, out_grad, zs, reps, send_a, send_b, R):
    T, C = out_grad.shape
    Ch = C // 2
    nb, nr = zs.shape[0], reps.shape[0]
    w = nr * R
    tc = min(512, Ch)
    nt = Ch // tc
    if w % 128 == 0:
        m, m_spec = mixer_out, pl.BlockSpec((T, w), lambda i, j, z, r: (0, z[i]))
    else:
        m = jnp.stack([lax.dynamic_slice_in_dim(mixer_out, zs[i] * w, w, 1) for i in range(nb)])
        m_spec = pl.BlockSpec((1, T, w), lambda i, j, z, r: (i, 0, 0))
    nk = 2 * nr - len(send_a) - len(send_b)
    out_shape = [jax.ShapeDtypeStruct((nb, len(s), R, Ch), BF) for s in (send_a, send_b)]
    out_shape += [jax.ShapeDtypeStruct((nb, R, Ch), F32)] * nk
    out_specs = [pl.BlockSpec((1, len(s), R, tc), lambda i, j, z, r: (i, 0, 0, j)) for s in (send_a, send_b)]
    out_specs += [pl.BlockSpec((1, R, tc), lambda i, j, z, r: (i, 0, j))] * nk
    outs = pl.pallas_call(
        functools.partial(grad_kernel, send_a, send_b, R),
        out_shape=out_shape,
        grid_spec=pltpu.PrefetchScalarGridSpec(
            num_scalar_prefetch=2,
            grid=(nb, nt),
            in_specs=[
                m_spec,
                pl.BlockSpec((T, tc), lambda i, j, z, r: (0, j)),
                pl.BlockSpec((T, tc), lambda i, j, z, r: (0, nt + j)),
            ],
            out_specs=out_specs,
            scratch_shapes=[pltpu.VMEM((w, tc), F32)],
        ),
        cost_estimate=pl.CostEstimate(
            flops=2 * nb * T * w * C, bytes_accessed=2 * T * (w * nb + C) + 6 * nb * w * C, transcendentals=0
        ),
        name="grad_blocks",
    )(zs, reps, m, out_grad, out_grad)
    keep_a = [r for r in range(nr) if r not in send_a]
    keep_b = [r for r in range(nr) if r not in send_b]
    kept = list(outs[2:])
    return (
        outs[0],
        {r: [kept.pop(0)] for r in keep_a},
        outs[1],
        {r: [kept.pop(0)] for r in keep_b},
    )


def place_kernel(n, has_prev, places, starts, *refs):
    pieces, out, bufs, sem_in, sem_out = refs[:n], refs[-n - 3], refs[-n - 2 : -2], refs[-2], refs[-1]
    loads, stores = [], []
    for k, (piece, buf, (index, rel, col)) in enumerate(zip(pieces, bufs, places)):
        src = piece if index is None else piece.at[index]
        R, Ch = src.shape
        row = pl.multiple_of(starts[rel], 8)
        loads.append(pltpu.make_async_copy(src, buf, sem_in.at[k]))
        stores.append(pltpu.make_async_copy(buf, out.at[pl.ds(row, R), pl.ds(col * Ch, Ch)], sem_out.at[k]))
    for load in loads:
        load.start()
    for load, store in zip(loads, stores):
        load.wait()
        store.start()
    for store in stores:
        store.wait()


def place(prev, shape, starts, items):
    arrays = [a for a, *_ in items]
    places = [tuple(rest) for _, *rest in items]
    n = len(arrays)
    extra = [] if prev is None else [prev]
    any_spec = pl.BlockSpec(memory_space=pl.ANY)
    return pl.pallas_call(
        functools.partial(place_kernel, n, prev is not None, places),
        out_shape=jax.ShapeDtypeStruct(shape, BF),
        in_specs=[pl.BlockSpec(memory_space=pltpu.SMEM)] + [any_spec] * (n + len(extra)),
        out_specs=any_spec,
        scratch_shapes=[pltpu.VMEM(a.shape[-2:], BF) for a in arrays] + [pltpu.SemaphoreType.DMA((n,))] * 2,
        input_output_aliases={} if prev is None else {n + 1: 0},
        name="place",
    )(starts, *arrays, *extra)


def total(parts):
    out = parts[0].astype(F32)
    for part in parts[1:]:
        out = out + part.astype(F32)
    return out


def halves(a, bit_set):
    n = a.shape[0] // 2
    low, high = a[:n], a[n:]
    return jnp.where(bit_set, high, low), jnp.where(bit_set, low, high)


def join(mine, other, bit_set):
    return jnp.where(bit_set, jnp.concatenate([other, mine]), jnp.concatenate([mine, other]))


def per_device(nf, nr, nt, mixer_out, out_grad, factors, weight, first_moment, second_moment):
    R, C = weight.shape
    Ch = C // 2
    K = factors.shape[1]
    fs, rep, tp = (lax.axis_index(a) for a in ("fs", "rep", "tp"))
    h = gray(fs)
    rep_bits, fs_bits, tp_bits = bits_of(nr), bits_of(nf), bits_of(nt)
    reps = jnp.stack([rep ^ r for r in range(nr)]).astype(jnp.int32)

    kt = K // nt
    part = lax.dynamic_slice_in_dim(factors, tp * kt, kt, 1)[None]
    for bit in rep_bits:
        part = join(part, swap(part, "rep", bit, nr), (rep & bit) != 0)
    for bit in reversed(fs_bits):
        part = join(part, swap(part, "fs", bit, nf), (h & bit) != 0)
    part = part.reshape([2] * len(fs_bits) + [nr * R, kt])

    def fs_index(z):
        g = gray(z)
        return tuple((g >> k) & 1 for k in range(len(fs_bits)))

    all_factors = jnp.concatenate([part[fs_index(z)] for z in range(nf)])
    mixed = jnp.dot(mixer_out, all_factors, preferred_element_type=F32).astype(BF)[None]
    for bit in tp_bits:
        mixed = join(mixed, swap(mixed, "tp", bit, nt), (tp & bit) != 0)
    mixed = jnp.concatenate([mixed[k] for k in range(nt)], axis=1)

    order_a, order_b = rep_bits, rep_bits[::-1]
    send_a = [r for r in range(nr) if r & order_a[0]]
    send_b = [r for r in range(nr) if r & order_b[0]]
    batches = [[r for r in range(nf) if r & (2 * bit - 1) == bit] for bit in fs_bits] + [[0]]
    arrived = {r: [] for r in range(nf)}
    for k, batch in enumerate(batches):
        zs = jnp.stack([ungray(h ^ r, nf) for r in batch]).astype(jnp.int32)
        first_a, keep_a, first_b, keep_b = grad_blocks(mixer_out, out_grad, zs, reps, send_a, send_b, R)
        sums = []
        for order, first, pieces in ((order_a, first_a, keep_a), (order_b, first_b, keep_b)):
            held = list(range(nr))
            for step, bit in enumerate(order):
                sent = [r for r in held if r & bit]
                if step == 0:
                    out = first
                else:
                    out = jnp.stack([total(pieces[r]) for r in sent], axis=1).astype(BF)
                got = swap(out, "rep", bit, nr)
                for i, r in enumerate(sent):
                    pieces[r ^ bit].append(got[:, i])
                held = [r for r in held if not r & bit]
            sums.append(total(pieces[0]))
        whole = jnp.concatenate(sums, axis=2)
        whole = [total([whole[i]] + arrived[r]) for i, r in enumerate(batch)]
        if k < len(fs_bits):
            got = swap(jnp.stack(whole).astype(BF), "fs", fs_bits[k], nf)
            for i, r in enumerate(batch):
                arrived[r ^ fs_bits[k]].append(got[i])
        else:
            gradient = whole[0]

    projected = lax.dot_general(mixed, out_grad, (((0,), (0,)), ((), ())), preferred_element_type=F32)
    projected = projected.reshape(nf, K // nf, C)
    projected = jnp.concatenate([projected[ungray(g, nf)][None] for g in range(nf)])
    rest = projected.reshape([2] * len(fs_bits) + [K // nf, C])
    for k, bit in enumerate(fs_bits):
        lead = jnp.moveaxis(rest, rest.ndim - 3, 0)
        keep, out = halves(lead, (h & bit) != 0)
        rest = (keep + swap(out.astype(BF), "fs", bit, nf).astype(F32))[0]
    rest = rest.reshape(nr, K // (nf * nr), C)
    for bit in reversed(rep_bits):
        keep, out = halves(rest, (rep & bit) != 0)
        rest = keep + swap(out.astype(BF), "rep", bit, nr).astype(F32)
    projected = rest[0]

    new_first = 0.8 * first_moment + 0.2 * projected
    new_second = 0.9 * second_moment + 0.1 * projected * projected
    direction = new_first / (jnp.sqrt(new_second) + 1e-08)
    dir_wide = direction.astype(BF).astype(F32)
    proj_wide = projected.astype(BF).astype(F32)
    sums = jnp.stack([jnp.sum(dir_wide * dir_wide), jnp.sum(proj_wide * proj_wide)])
    for axis, n, bits in (("tp", nt, tp_bits), ("rep", nr, rep_bits), ("fs", nf, fs_bits)):
        for bit in bits:
            sums = sums + swap(sums, axis, bit, n)
    scale_ratio = jnp.sqrt(sums[0]) / jnp.sqrt(sums[1] + 1e-06)

    mix = (dir_wide - scale_ratio * proj_wide).astype(BF)[None]
    for bit in reversed(fs_bits):
        mix = join(mix, swap(mix, "fs", bit, nf), (h & bit) != 0)
    for bit in rep_bits:
        mix = join(mix, swap(mix, "rep", bit, nr), (rep & bit) != 0)
    mix = mix.reshape([nr] + [2] * len(fs_bits) + [K // (nf * nr), C])
    mix = jnp.concatenate([mix[(r,) + fs_index(z)] for z in range(nf) for r in range(nr)])

    update = scale_ratio * gradient + jnp.dot(factors, mix, preferred_element_type=F32)
    new_weight = weight - 0.01 * update
    low = new_weight.astype(BF)

    copy = None
    held = {0: low}
    pending = [0]
    steps = []
    for k in reversed(range(len(fs_bits))):
        for r in list(held):
            held[r ^ fs_bits[k]] = swap(held[r], "fs", fs_bits[k], nf)
    for r, block in held.items():
        items = []
        for col, order in ((0, order_a[::-1]), (1, order_b[::-1])):
            mine = block[:, col * Ch : (col + 1) * Ch]
            items.append((mine, None, 0, col))
            have, rels = mine[None], [0]
            for step, bit in enumerate(order):
                got = swap(have, "rep", bit, nr)
                more = [q ^ bit for q in rels]
                items += [(got, i, q, col) for i, q in enumerate(more)]
                have, rels = (jnp.concatenate([have, got]) if step < len(order) - 1 else None), rels + more
        arrays, seen = [], {}
        starts = ((ungray(h ^ r, nf) * nr + reps) * R).astype(jnp.int32)
        copy = place(copy, (nf * nr * R, C), starts, items)
    return (new_weight, update, new_first, new_second, copy)


def solution(mesh):
    sizes = mesh.shape
    in_specs = (
        P(("fs", "rep"), None),
        P(("fs", "rep"), "tp"),
        P(("fs", "rep"), None),
        P(("fs", "rep"), "tp"),
        P(("fs", "rep"), "tp"),
        P(("fs", "rep"), "tp"),
    )
    out_specs = (
        P(("fs", "rep"), "tp"),
        P(("fs", "rep"), "tp"),
        P(("fs", "rep"), "tp"),
        P(("fs", "rep"), "tp"),
        P(None, "tp"),
    )
    return jax.shard_map(
        functools.partial(per_device, sizes["fs"], sizes["rep"], sizes["tp"]),
        mesh=mesh,
        in_specs=in_specs,
        out_specs=out_specs,
        check_vma=False,
    )
```

```python
import functools

import jax
import jax.numpy as jnp
from jax import lax
from jax.experimental import pallas as pl
from jax.experimental.pallas import tpu as pltpu
from jax.sharding import PartitionSpec as P


BF = jnp.bfloat16
F32 = jnp.float32


def gray(z):
    return z ^ (z >> 1)


def ungray(h, n):
    z, step = h, 1
    while step < n:
        z = z ^ (z >> step)
        step *= 2
    return z


def bits_of(n):
    return [1 << k for k in range(n.bit_length() - 1)]


def swap(a, axis, bit, n):
    if axis == "fs":
        pairs = [(z, ungray(gray(z) ^ bit, n)) for z in range(n)]
    else:
        pairs = [(i, i ^ bit) for i in range(n)]
    return lax.ppermute(a, axis, pairs)


def grad_kernel(send_a, send_b, R, nr, zs, reps, m, oa, ob, *refs):
    acc, sems = refs[-2], refs[-1]
    count = (len(refs) - 2) // 2
    outs, bufs = refs[:count], refs[count:-2]
    per = 2 + 2 * nr - len(send_a) - len(send_b)
    chunks = count // per
    copies = [pltpu.make_async_copy(buf, out, sems.at[k]) for k, (buf, out) in enumerate(zip(bufs, outs))]
    for c in range(chunks):

        @pl.when(pl.program_id(0) == c)
        def _():
            sends, keeps = bufs[c * per : c * per + 2], list(bufs[c * per + 2 : (c + 1) * per])
            for send, out, o in ((send_a, sends[0], oa), (send_b, sends[1], ob)):
                acc[...] = lax.dot_general(
                    m[...].reshape(m.shape[-2:]), o[...], (((0,), (0,)), ((), ())), preferred_element_type=F32
                )
                for rel in range(nr):
                    rows = acc[pl.ds(pl.multiple_of(reps[rel] * R, 8), R), :]
                    if rel in send:
                        out[send.index(rel)] = rows.astype(BF)
                    else:
                        keeps.pop(0)[...] = rows
            for copy in copies[c * per : (c + 1) * per]:
                copy.start()

    @pl.when(pl.program_id(0) == chunks - 1)
    def _():
        for copy in copies:
            copy.wait()


def grad_blocks(mixer_out, out_grad, zs, reps, send_a, send_b, R):
    T, C = out_grad.shape
    Ch = C // 2
    nb, nr = zs.shape[0], reps.shape[0]
    w = nr * R
    if w % 128 == 0:
        m, m_spec = mixer_out, pl.BlockSpec((T, w), lambda i, z, r: (0, z[i]))
    else:
        m = jnp.stack([lax.dynamic_slice_in_dim(mixer_out, zs[i] * w, w, 1) for i in range(nb)])
        m_spec = pl.BlockSpec((1, T, w), lambda i, z, r: (i, 0, 0))
    nk = 2 * nr - len(send_a) - len(send_b)
    out_shape = []
    for _ in range(nb):
        out_shape += [jax.ShapeDtypeStruct((len(q), R, Ch), BF) for q in (send_a, send_b)]
        out_shape += [jax.ShapeDtypeStruct((R, Ch), F32)] * nk
    out_specs = [pl.BlockSpec(memory_space=pl.ANY)] * len(out_shape)
    bufs = [pltpu.VMEM(a.shape, a.dtype) for a in out_shape]
    outs = pl.pallas_call(
        functools.partial(grad_kernel, send_a, send_b, R, nr),
        out_shape=out_shape,
        grid_spec=pltpu.PrefetchScalarGridSpec(
            num_scalar_prefetch=2,
            grid=(nb,),
            in_specs=[
                m_spec,
                pl.BlockSpec((T, Ch), lambda i, z, r: (0, 0)),
                pl.BlockSpec((T, Ch), lambda i, z, r: (0, 1)),
            ],
            out_specs=out_specs,
            scratch_shapes=bufs + [pltpu.VMEM((w, Ch), F32), pltpu.SemaphoreType.DMA((len(bufs),))],
        ),
        cost_estimate=pl.CostEstimate(
            flops=2 * nb * T * w * C, bytes_accessed=2 * T * (w * nb + C) + 6 * nb * w * C, transcendentals=0
        ),
        name="grad_blocks",
    )(zs, reps, m, out_grad, out_grad)
    keep_a = [r for r in range(nr) if r not in send_a]
    keep_b = [r for r in range(nr) if r not in send_b]
    result, outs = [], list(outs)
    for _ in range(nb):
        first_a, first_b = outs.pop(0), outs.pop(0)
        result.append(
            (first_a, {r: [outs.pop(0)] for r in keep_a}, first_b, {r: [outs.pop(0)] for r in keep_b})
        )
    return result


def place_kernel(n, nr, places, starts, factors, mix, *refs):
    pieces, out = refs[:n], refs[-2 * n - 8]
    lbuf = refs[-2 * n - 7]
    fbuf, mbuf, bufs, done = refs[-2 * n - 6], refs[-2 * n - 5], refs[-2 * n - 4 : -n - 4], refs[-n - 4 : -4]
    sem_f, sem_m, sem_in, sem_out = refs[-4:]
    R = fbuf.shape[1]
    mix_load = pltpu.make_async_copy(mix, mbuf, sem_m.at[0])
    mix_load.start()
    block_load = pltpu.make_async_copy(factors, fbuf, sem_f.at[0])
    block_load.start()
    loads, stores = [], []
    for k, (piece, (rel, col, width)) in enumerate(zip(pieces, places)):
        row = pl.multiple_of(starts[rel] * R, 8)
        loads.append(pltpu.make_async_copy(piece, bufs[k], sem_in.at[k]))
        stores.append(pltpu.make_async_copy(done[k], out.at[pl.ds(row, R), pl.ds(col, width)], sem_out.at[k]))
    for load in loads:
        load.start()
    block_load.wait()
    mix_load.wait()
    chunk, base = -1, None
    for k, (rel, col, width) in enumerate(places):
        if rel // nr != chunk:
            chunk = rel // nr
            base = starts[chunk * nr] // nr * nr
            rows = fbuf[pl.ds(base, nr)].reshape(nr * R, fbuf.shape[2])
            lbuf[...] = 0.01 * jnp.dot(rows, mbuf[...], preferred_element_type=F32)
        row = pl.multiple_of((starts[rel] - base) * R, 8)
        loads[k].wait()
        done[k][...] = (bufs[k][...].astype(F32) - lbuf[pl.ds(row, R), col : col + width]).astype(BF)
        stores[k].start()
    for store in stores:
        store.wait()


def place(prev, shape, starts, factors, mix, nr, items):
    arrays = [a for a, *_ in items]
    places = [(rel, col, a.shape[1]) for a, rel, col in items]
    n = len(arrays)
    extra = [] if prev is None else [prev]
    any_spec = pl.BlockSpec(memory_space=pl.ANY)
    bufs = [pltpu.VMEM(a.shape, BF) for a in arrays]
    dma = pltpu.SemaphoreType.DMA
    return pl.pallas_call(
        functools.partial(place_kernel, n, nr, places),
        out_shape=jax.ShapeDtypeStruct(shape, BF),
        in_specs=[pl.BlockSpec(memory_space=pltpu.SMEM)] + [any_spec] * (n + 2 + len(extra)),
        out_specs=any_spec,
        scratch_shapes=[pltpu.VMEM((nr * arrays[0].shape[0], shape[1]), F32), pltpu.VMEM(factors.shape, BF), pltpu.VMEM(mix.shape, BF)]
        + bufs
        + bufs
        + [dma((1,)), dma((1,)), dma((n,)), dma((n,))],
        input_output_aliases={} if prev is None else {n + 3: 0},
        name="place",
    )(starts, factors, mix, *arrays, *extra)


def total(parts):
    parts = [p[0][p[1]] if isinstance(p, tuple) else p for p in parts]
    out = parts[0].astype(F32)
    for part in parts[1:]:
        out = out + part.astype(F32)
    return out


def sum_kernel(na, nb, *refs):
    out = refs[-1]
    Ch = out.shape[1] // 2
    for half, (low, high) in enumerate(((0, na), (na, na + nb))):
        cols = slice(half * Ch, (half + 1) * Ch)
        acc = refs[low][...].astype(F32)
        for ref in refs[low + 1 : high]:
            acc = acc + ref[...].astype(F32)
        for ref in refs[na + nb : -1]:
            acc = acc + ref[:, cols].astype(F32)
        out[:, cols] = acc.astype(out.dtype)


def plane_sum(parts, arrived, dtype):
    arrays, specs = [], []
    for part in parts[0] + parts[1]:
        if isinstance(part, tuple):
            part, i = part
            specs.append(pl.BlockSpec((None,) + part.shape[1:], lambda g, k=i: (k, 0, 0)))
        else:
            specs.append(pl.BlockSpec(part.shape, lambda g: (0, 0)))
        arrays.append(part)
    R, Ch = arrays[0].shape
    for a in arrived:
        specs.append(pl.BlockSpec(a.shape, lambda g: (0, 0)))
        arrays.append(a)
    return pl.pallas_call(
        functools.partial(sum_kernel, len(parts[0]), len(parts[1])),
        out_shape=jax.ShapeDtypeStruct((R, 2 * Ch), dtype),
        grid=(1,),
        in_specs=specs,
        out_specs=pl.BlockSpec((R, 2 * Ch), lambda g: (0, 0)),
        name="plane_sum",
    )(*arrays)


def halves(a, bit_set):
    n = a.shape[0] // 2
    low, high = a[:n], a[n:]
    return jnp.where(bit_set, high, low), jnp.where(bit_set, low, high)


def join(mine, other, bit_set):
    return jnp.where(bit_set, jnp.concatenate([other, mine]), jnp.concatenate([mine, other]))


def per_device(nf, nr, nt, mixer_out, out_grad, factors, weight, first_moment, second_moment):
    return body(nf, nr, nt, mixer_out, out_grad, factors, weight, first_moment, second_moment)


def body(nf, nr, nt, mixer_out, out_grad, factors, weight, first_moment, second_moment):
    R, C = weight.shape
    Ch = C // 2
    K = factors.shape[1]
    fs, rep, tp = (lax.axis_index(a) for a in ("fs", "rep", "tp"))
    h = gray(fs)
    rep_bits, fs_bits, tp_bits = bits_of(nr), bits_of(nf), bits_of(nt)
    reps = jnp.stack([rep ^ r for r in range(nr)]).astype(jnp.int32)

    kt = K // nt
    part = lax.dynamic_slice_in_dim(factors, tp * kt, kt, 1)[None]
    for bit in rep_bits:
        part = join(part, swap(part, "rep", bit, nr), (rep & bit) != 0)
    for bit in reversed(fs_bits):
        part = join(part, swap(part, "fs", bit, nf), (h & bit) != 0)
    part = part.reshape([2] * len(fs_bits) + [nr * R, kt])

    def fs_index(z):
        g = gray(z)
        return tuple((g >> k) & 1 for k in range(len(fs_bits)))

    all_factors = jnp.concatenate([part[fs_index(z)] for z in range(nf)])
    whole_factors = all_factors[None]
    for bit in tp_bits:
        whole_factors = join(whole_factors, swap(whole_factors, "tp", bit, nt), (tp & bit) != 0)
    whole_factors = jnp.concatenate([whole_factors[k].reshape(nf * nr, R, kt) for k in range(nt)], axis=2)
    mixed = jnp.dot(mixer_out, all_factors, preferred_element_type=F32).astype(BF)[None]
    for bit in tp_bits:
        mixed = join(mixed, swap(mixed, "tp", bit, nt), (tp & bit) != 0)
    mixed = jnp.concatenate([mixed[k] for k in range(nt)], axis=1)

    order_a, order_b = rep_bits, rep_bits[::-1]
    send_a = [r for r in range(nr) if r & order_a[0]]
    send_b = [r for r in range(nr) if r & order_b[0]]
    rels = list(range(nf))[::-1]
    groups = [rels[i : i + 2] for i in range(0, nf, 2)]
    blocks = {}
    for group in groups:
        zs = jnp.stack([ungray(h ^ r, nf) for r in group]).astype(jnp.int32)
        made = grad_blocks(mixer_out, out_grad, zs, reps, send_a, send_b, R)
        blocks.update(zip(group, made))
    arrived = {r: [] for r in range(nf)}
    for rel in rels:
        first_a, keep_a, first_b, keep_b = blocks[rel]
        parts = []
        for order, first, pieces in ((order_a, first_a, keep_a), (order_b, first_b, keep_b)):
            held = list(range(nr))
            for step, bit in enumerate(order):
                sent = [r for r in held if r & bit]
                out = jnp.stack([total(pieces[r]) for r in sent]).astype(BF) if step else first
                got = swap(out, "rep", bit, nr)
                for i, r in enumerate(sent):
                    pieces[r ^ bit].append((got, i))
                held = [r for r in held if not r & bit]
            parts.append(pieces[0])
        whole = plane_sum(parts, arrived[rel], BF if rel else F32)
        if rel:
            bit = rel & -rel
            arrived[rel ^ bit].append(swap(whole, "fs", bit, nf))
        else:
            gradient = whole

    projected = lax.dot_general(mixed, out_grad, (((0,), (0,)), ((), ())), preferred_element_type=F32)
    projected = projected.reshape(nf, K // nf, C)
    projected = jnp.concatenate([projected[ungray(g, nf)][None] for g in range(nf)])
    rest = projected.reshape([2] * len(fs_bits) + [K // nf, C])
    for bit in fs_bits:
        lead = jnp.moveaxis(rest, rest.ndim - 3, 0)
        keep, out = halves(lead, (h & bit) != 0)
        rest = (keep + swap(out.astype(BF), "fs", bit, nf).astype(F32))[0]
    rest = rest.reshape(nr, K // (nf * nr), C)
    for bit in reversed(rep_bits):
        keep, out = halves(rest, (rep & bit) != 0)
        rest = keep + swap(out.astype(BF), "rep", bit, nr).astype(F32)
    projected = rest[0]

    new_first = 0.8 * first_moment + 0.2 * projected
    new_second = 0.9 * second_moment + 0.1 * projected * projected
    direction = new_first / (jnp.sqrt(new_second) + 1e-08)
    dir_wide = direction.astype(BF).astype(F32)
    proj_wide = projected.astype(BF).astype(F32)
    sums = jnp.stack([jnp.sum(dir_wide * dir_wide, 0), jnp.sum(proj_wide * proj_wide, 0)])
    for axis, n, bits in (("tp", nt, tp_bits), ("rep", nr, rep_bits), ("fs", nf, fs_bits)):
        for bit in bits:
            sums = sums + swap(sums, axis, bit, n)
    sums = jnp.sum(sums, 1)
    scale_ratio = jnp.sqrt(sums[0]) / jnp.sqrt(sums[1] + 1e-06)

    low = (weight - 0.01 * (scale_ratio * gradient)).astype(BF)
    held = {0: low}
    for k in reversed(range(len(fs_bits))):
        for r in list(held):
            held[r ^ fs_bits[k]] = swap(held[r], "fs", fs_bits[k], nf)
    gathered = {}
    for r, block in held.items():
        have = {0: [(block, 0)]}
        if len(rep_bits) == 2:
            one, two = rep_bits
            from_one = swap(block, "rep", one, nr)
            from_two = swap(block, "rep", two, nr)
            left = swap(from_two[:, :Ch], "rep", one, nr)
            right = swap(from_one[:, Ch:], "rep", two, nr)
            have = {0: [(block, 0)], one: [(from_one, 0)], two: [(from_two, 0)], one | two: [(left, 0), (right, Ch)]}
        else:
            for bit in rep_bits:
                for q in list(have):
                    have[q ^ bit] = [(swap(have[q][0][0], "rep", bit, nr), 0)]
        gathered[r] = [(a, q, col) for q in sorted(have) for a, col in have[q]]

    mix = (dir_wide - scale_ratio * proj_wide).astype(BF)[None]
    for bit in reversed(fs_bits):
        mix = join(mix, swap(mix, "fs", bit, nf), (h & bit) != 0)
    mix = mix.reshape([2] * len(fs_bits) + [K // (nf * nr), C])
    mix = jnp.stack([mix[fs_index(z)] for z in range(nf)])[None]
    mixes = []
    for order, cols in ((rep_bits, slice(0, Ch)), (rep_bits[::-1], slice(Ch, C))):
        half = mix[..., cols]
        for bit in order:
            half = join(half, swap(half, "rep", bit, nr), (rep & bit) != 0)
        half = half.reshape([2] * len(order) + list(half.shape[1:]))
        spots = [[(r >> (bit.bit_length() - 1)) & 1 for bit in reversed(order)] for r in range(nr)]
        mixes.append(jnp.stack([half[tuple(spot)] for spot in spots], axis=1).reshape(K, Ch))
    mix = jnp.concatenate(mixes, axis=1)

    mix, gradient, weight, scale_ratio = lax.optimization_barrier((mix, gradient, weight, scale_ratio))
    update = scale_ratio * gradient + jnp.dot(factors, mix, preferred_element_type=F32)
    new_weight = weight - 0.01 * update

    copy = None
    for group in [[r] for r in range(nf)]:
        starts = jnp.concatenate([ungray(h ^ r, nf) * nr + reps for r in group]).astype(jnp.int32)
        items = [(a, k * nr + q, col) for k, r in enumerate(group) for a, q, col in gathered[r]]
        copy = place(copy, (nf * nr * R, C), starts, whole_factors, mix, nr, items)
    return (new_weight, update, new_first, new_second, copy)


def solution(mesh):
    sizes = mesh.shape
    in_specs = (
        P(("fs", "rep"), None),
        P(("fs", "rep"), "tp"),
        P(("fs", "rep"), None),
        P(("fs", "rep"), "tp"),
        P(("fs", "rep"), "tp"),
        P(("fs", "rep"), "tp"),
    )
    out_specs = (
        P(("fs", "rep"), "tp"),
        P(("fs", "rep"), "tp"),
        P(("fs", "rep"), "tp"),
        P(("fs", "rep"), "tp"),
        P(None, "tp"),
    )
    return jax.shard_map(
        functools.partial(per_device, sizes["fs"], sizes["rep"], sizes["tp"]),
        mesh=mesh,
        in_specs=in_specs,
        out_specs=out_specs,
        check_vma=False,
    )
```

```python
import functools

import jax
import jax.numpy as jnp
from jax import lax
from jax.experimental import pallas as pl
from jax.experimental.pallas import tpu as pltpu
from jax.sharding import PartitionSpec as P


BF = jnp.bfloat16
F32 = jnp.float32


def gray(z):
    return z ^ (z >> 1)


def ungray(h, n):
    z, step = h, 1
    while step < n:
        z = z ^ (z >> step)
        step *= 2
    return z


def bits_of(n):
    return [1 << k for k in range(n.bit_length() - 1)]


def swap(a, axis, bit, n):
    if axis == "fs":
        pairs = [(z, ungray(gray(z) ^ bit, n)) for z in range(n)]
    else:
        pairs = [(i, i ^ bit) for i in range(n)]
    return lax.ppermute(a, axis, pairs)


def grad_kernel(send_a, send_b, R, nr, zs, reps, m, oa, ob, *refs):
    acc, sems = refs[-2], refs[-1]
    count = (len(refs) - 2) // 2
    outs, bufs = refs[:count], refs[count:-2]
    per = 2 + 2 * nr - len(send_a) - len(send_b)
    chunks = count // per
    copies = [pltpu.make_async_copy(buf, out, sems.at[k]) for k, (buf, out) in enumerate(zip(bufs, outs))]
    for c in range(chunks):

        @pl.when(pl.program_id(0) == c)
        def _():
            sends, keeps = bufs[c * per : c * per + 2], list(bufs[c * per + 2 : (c + 1) * per])
            for send, out, o in ((send_a, sends[0], oa), (send_b, sends[1], ob)):
                acc[...] = lax.dot_general(
                    m[...].reshape(m.shape[-2:]), o[...], (((0,), (0,)), ((), ())), preferred_element_type=F32
                )
                for rel in range(nr):
                    rows = acc[pl.ds(pl.multiple_of(reps[rel] * R, 8), R), :]
                    if rel in send:
                        out[send.index(rel)] = rows.astype(BF)
                    else:
                        keeps.pop(0)[...] = rows
            for copy in copies[c * per : (c + 1) * per]:
                copy.start()

    @pl.when(pl.program_id(0) == chunks - 1)
    def _():
        for copy in copies:
            copy.wait()


def grad_blocks(mixer_out, out_grad, zs, reps, send_a, send_b, R):
    T, C = out_grad.shape
    Ch = C // 2
    nb, nr = zs.shape[0], reps.shape[0]
    w = nr * R
    if w % 128 == 0:
        m, m_spec = mixer_out, pl.BlockSpec((T, w), lambda i, z, r: (0, z[i]))
    else:
        m = jnp.stack([lax.dynamic_slice_in_dim(mixer_out, zs[i] * w, w, 1) for i in range(nb)])
        m_spec = pl.BlockSpec((1, T, w), lambda i, z, r: (i, 0, 0))
    nk = 2 * nr - len(send_a) - len(send_b)
    out_shape = []
    for _ in range(nb):
        out_shape += [jax.ShapeDtypeStruct((len(q), R, Ch), BF) for q in (send_a, send_b)]
        out_shape += [jax.ShapeDtypeStruct((R, Ch), F32)] * nk
    out_specs = [pl.BlockSpec(memory_space=pl.ANY)] * len(out_shape)
    bufs = [pltpu.VMEM(a.shape, a.dtype) for a in out_shape]
    outs = pl.pallas_call(
        functools.partial(grad_kernel, send_a, send_b, R, nr),
        out_shape=out_shape,
        grid_spec=pltpu.PrefetchScalarGridSpec(
            num_scalar_prefetch=2,
            grid=(nb,),
            in_specs=[
                m_spec,
                pl.BlockSpec((T, Ch), lambda i, z, r: (0, 0)),
                pl.BlockSpec((T, Ch), lambda i, z, r: (0, 1)),
            ],
            out_specs=out_specs,
            scratch_shapes=bufs + [pltpu.VMEM((w, Ch), F32), pltpu.SemaphoreType.DMA((len(bufs),))],
        ),
        cost_estimate=pl.CostEstimate(
            flops=2 * nb * T * w * C, bytes_accessed=2 * T * (w * nb + C) + 6 * nb * w * C, transcendentals=0
        ),
        name="grad_blocks",
    )(zs, reps, m, out_grad, out_grad)
    keep_a = [r for r in range(nr) if r not in send_a]
    keep_b = [r for r in range(nr) if r not in send_b]
    result, outs = [], list(outs)
    for _ in range(nb):
        first_a, first_b = outs.pop(0), outs.pop(0)
        result.append(
            (first_a, {r: [outs.pop(0)] for r in keep_a}, first_b, {r: [outs.pop(0)] for r in keep_b})
        )
    return result


def place_kernel(n, nr, places, starts, factors, mix, *refs):
    pieces, out = refs[:n], refs[-2 * n - 8]
    lbuf = refs[-2 * n - 7]
    fbuf, mbuf, bufs, done = refs[-2 * n - 6], refs[-2 * n - 5], refs[-2 * n - 4 : -n - 4], refs[-n - 4 : -4]
    sem_f, sem_m, sem_in, sem_out = refs[-4:]
    R = fbuf.shape[1]
    mix_load = pltpu.make_async_copy(mix, mbuf, sem_m.at[0])
    mix_load.start()
    block_load = pltpu.make_async_copy(factors, fbuf, sem_f.at[0])
    block_load.start()
    loads, stores = [], []
    for k, (piece, (rel, col, width)) in enumerate(zip(pieces, places)):
        row = pl.multiple_of(starts[rel] * R, 8)
        loads.append(pltpu.make_async_copy(piece, bufs[k], sem_in.at[k]))
        stores.append(pltpu.make_async_copy(done[k], out.at[pl.ds(row, R), pl.ds(col, width)], sem_out.at[k]))
    for load in loads:
        load.start()
    block_load.wait()
    mix_load.wait()
    chunk, base = -1, None
    for k, (rel, col, width) in enumerate(places):
        if rel // nr != chunk:
            chunk = rel // nr
            base = starts[chunk * nr] // nr * nr
            rows = fbuf[pl.ds(base, nr)].reshape(nr * R, fbuf.shape[2])
            lbuf[...] = 0.01 * jnp.dot(rows, mbuf[...], preferred_element_type=F32)
        row = pl.multiple_of((starts[rel] - base) * R, 8)
        loads[k].wait()
        done[k][...] = (bufs[k][...].astype(F32) - lbuf[pl.ds(row, R), col : col + width]).astype(BF)
        stores[k].start()
    for store in stores:
        store.wait()


def place(prev, shape, starts, factors, mix, nr, items):
    arrays = [a for a, *_ in items]
    places = [(rel, col, a.shape[1]) for a, rel, col in items]
    n = len(arrays)
    extra = [] if prev is None else [prev]
    any_spec = pl.BlockSpec(memory_space=pl.ANY)
    bufs = [pltpu.VMEM(a.shape, BF) for a in arrays]
    dma = pltpu.SemaphoreType.DMA
    return pl.pallas_call(
        functools.partial(place_kernel, n, nr, places),
        out_shape=jax.ShapeDtypeStruct(shape, BF),
        in_specs=[pl.BlockSpec(memory_space=pltpu.SMEM)] + [any_spec] * (n + 2 + len(extra)),
        out_specs=any_spec,
        scratch_shapes=[pltpu.VMEM((nr * arrays[0].shape[0], shape[1]), F32), pltpu.VMEM(factors.shape, BF), pltpu.VMEM(mix.shape, BF)]
        + bufs
        + bufs
        + [dma((1,)), dma((1,)), dma((n,)), dma((n,))],
        input_output_aliases={} if prev is None else {n + 3: 0},
        name="place",
    )(starts, factors, mix, *arrays, *extra)


def total(parts):
    parts = [p[0][p[1]] if isinstance(p, tuple) else p for p in parts]
    out = parts[0].astype(F32)
    for part in parts[1:]:
        out = out + part.astype(F32)
    return out


def sum_kernel(na, nb, *refs):
    out = refs[-1]
    Ch = out.shape[1] // 2
    for half, (low, high) in enumerate(((0, na), (na, na + nb))):
        cols = slice(half * Ch, (half + 1) * Ch)
        acc = refs[low][...].astype(F32)
        for ref in refs[low + 1 : high]:
            acc = acc + ref[...].astype(F32)
        for ref in refs[na + nb : -1]:
            acc = acc + ref[:, cols].astype(F32)
        out[:, cols] = acc.astype(out.dtype)


def plane_sum(parts, arrived, dtype):
    arrays, specs = [], []
    for part in parts[0] + parts[1]:
        if isinstance(part, tuple):
            part, i = part
            specs.append(pl.BlockSpec((None,) + part.shape[1:], lambda g, k=i: (k, 0, 0)))
        else:
            specs.append(pl.BlockSpec(part.shape, lambda g: (0, 0)))
        arrays.append(part)
    R, Ch = arrays[0].shape
    for a in arrived:
        specs.append(pl.BlockSpec(a.shape, lambda g: (0, 0)))
        arrays.append(a)
    return pl.pallas_call(
        functools.partial(sum_kernel, len(parts[0]), len(parts[1])),
        out_shape=jax.ShapeDtypeStruct((R, 2 * Ch), dtype),
        grid=(1,),
        in_specs=specs,
        out_specs=pl.BlockSpec((R, 2 * Ch), lambda g: (0, 0)),
        name="plane_sum",
    )(*arrays)


def halves(a, bit_set):
    n = a.shape[0] // 2
    low, high = a[:n], a[n:]
    return jnp.where(bit_set, high, low), jnp.where(bit_set, low, high)


def join(mine, other, bit_set):
    return jnp.where(bit_set, jnp.concatenate([other, mine]), jnp.concatenate([mine, other]))


def per_device(nf, nr, nt, mixer_out, out_grad, factors, weight, first_moment, second_moment):
    return body(nf, nr, nt, mixer_out, out_grad, factors, weight, first_moment, second_moment)


def body(nf, nr, nt, mixer_out, out_grad, factors, weight, first_moment, second_moment):
    R, C = weight.shape
    Ch = C // 2
    K = factors.shape[1]
    fs, rep, tp = (lax.axis_index(a) for a in ("fs", "rep", "tp"))
    h = gray(fs)
    rep_bits, fs_bits, tp_bits = bits_of(nr), bits_of(nf), bits_of(nt)
    reps = jnp.stack([rep ^ r for r in range(nr)]).astype(jnp.int32)

    kt = K // nt
    part = lax.dynamic_slice_in_dim(factors, tp * kt, kt, 1)[None]
    for bit in rep_bits:
        part = join(part, swap(part, "rep", bit, nr), (rep & bit) != 0)
    for bit in reversed(fs_bits):
        part = join(part, swap(part, "fs", bit, nf), (h & bit) != 0)
    part = part.reshape([2] * len(fs_bits) + [nr * R, kt])

    def fs_index(z):
        g = gray(z)
        return tuple((g >> k) & 1 for k in range(len(fs_bits)))

    all_factors = jnp.concatenate([part[fs_index(z)] for z in range(nf)])
    whole_factors = all_factors[None]
    for bit in tp_bits:
        whole_factors = join(whole_factors, swap(whole_factors, "tp", bit, nt), (tp & bit) != 0)
    whole_factors = jnp.concatenate([whole_factors[k].reshape(nf * nr, R, kt) for k in range(nt)], axis=2)
    mixed = jnp.dot(mixer_out, all_factors, preferred_element_type=F32).astype(BF)[None]
    for bit in tp_bits:
        mixed = join(mixed, swap(mixed, "tp", bit, nt), (tp & bit) != 0)
    mixed = jnp.concatenate([mixed[k] for k in range(nt)], axis=1)

    order_a, order_b = rep_bits, rep_bits[::-1]
    send_a = [r for r in range(nr) if r & order_a[0]]
    send_b = [r for r in range(nr) if r & order_b[0]]
    rels = list(range(nf))[::-1]
    groups = [rels[i : i + 2] for i in range(0, nf, 2)]
    blocks = {}
    for group in groups:
        zs = jnp.stack([ungray(h ^ r, nf) for r in group]).astype(jnp.int32)
        made = grad_blocks(mixer_out, out_grad, zs, reps, send_a, send_b, R)
        blocks.update(zip(group, made))
    arrived = {r: [] for r in range(nf)}
    for rel in rels:
        first_a, keep_a, first_b, keep_b = blocks[rel]
        parts = []
        for order, first, pieces in ((order_a, first_a, keep_a), (order_b, first_b, keep_b)):
            held = list(range(nr))
            for step, bit in enumerate(order):
                sent = [r for r in held if r & bit]
                out = jnp.stack([total(pieces[r]) for r in sent]).astype(BF) if step else first
                got = swap(out, "rep", bit, nr)
                for i, r in enumerate(sent):
                    pieces[r ^ bit].append((got, i))
                held = [r for r in held if not r & bit]
            parts.append(pieces[0])
        whole = plane_sum(parts, arrived[rel], BF if rel else F32)
        if rel:
            bit = rel & -rel
            arrived[rel ^ bit].append(swap(whole, "fs", bit, nf))
        else:
            gradient = whole

    projected = lax.dot_general(mixed, out_grad, (((0,), (0,)), ((), ())), preferred_element_type=F32)
    projected = projected.reshape(nf, K // nf, C)
    projected = jnp.concatenate([projected[ungray(g, nf)][None] for g in range(nf)])
    rest = projected.reshape([2] * len(fs_bits) + [K // nf, C])
    for bit in fs_bits:
        lead = jnp.moveaxis(rest, rest.ndim - 3, 0)
        keep, out = halves(lead, (h & bit) != 0)
        rest = (keep + swap(out.astype(BF), "fs", bit, nf).astype(F32))[0]
    rest = rest.reshape(nr, K // (nf * nr), C)
    for bit in reversed(rep_bits):
        keep, out = halves(rest, (rep & bit) != 0)
        rest = keep + swap(out.astype(BF), "rep", bit, nr).astype(F32)
    projected = rest[0]

    new_first = 0.8 * first_moment + 0.2 * projected
    new_second = 0.9 * second_moment + 0.1 * projected * projected
    direction = new_first / (jnp.sqrt(new_second) + 1e-08)
    dir_wide = direction.astype(BF).astype(F32)
    proj_wide = projected.astype(BF).astype(F32)
    sums = jnp.stack([jnp.sum(dir_wide * dir_wide, 0), jnp.sum(proj_wide * proj_wide, 0)])
    for axis, n, bits in (("tp", nt, tp_bits), ("rep", nr, rep_bits), ("fs", nf, fs_bits)):
        for bit in bits:
            sums = sums + swap(sums, axis, bit, n)
    sums = jnp.sum(sums, 1)
    scale_ratio = jnp.sqrt(sums[0]) / jnp.sqrt(sums[1] + 1e-06)

    low = (weight - 0.01 * (scale_ratio * gradient)).astype(BF)
    held = {0: low}
    for k in reversed(range(len(fs_bits))):
        for r in list(held):
            held[r ^ fs_bits[k]] = swap(held[r], "fs", fs_bits[k], nf)
    gathered = {}
    for r, block in held.items():
        have = {0: [(block, 0)]}
        if len(rep_bits) == 2:
            one, two = rep_bits
            from_one = swap(block, "rep", one, nr)
            from_two = swap(block, "rep", two, nr)
            left = swap(from_two[:, :Ch], "rep", one, nr)
            right = swap(from_one[:, Ch:], "rep", two, nr)
            have = {0: [(block, 0)], one: [(from_one, 0)], two: [(from_two, 0)], one | two: [(left, 0), (right, Ch)]}
        else:
            for bit in rep_bits:
                for q in list(have):
                    have[q ^ bit] = [(swap(have[q][0][0], "rep", bit, nr), 0)]
        gathered[r] = [(a, q, col) for q in sorted(have) for a, col in have[q]]

    mix = (dir_wide - scale_ratio * proj_wide).astype(BF)[None]
    for bit in reversed(fs_bits):
        mix = join(mix, swap(mix, "fs", bit, nf), (h & bit) != 0)
    mix = mix.reshape([2] * len(fs_bits) + [K // (nf * nr), C])
    mix = jnp.stack([mix[fs_index(z)] for z in range(nf)])[None]
    mixes = []
    for order, cols in ((rep_bits, slice(0, Ch)), (rep_bits[::-1], slice(Ch, C))):
        half = mix[..., cols]
        for bit in order:
            half = join(half, swap(half, "rep", bit, nr), (rep & bit) != 0)
        half = half.reshape([2] * len(order) + list(half.shape[1:]))
        spots = [[(r >> (bit.bit_length() - 1)) & 1 for bit in reversed(order)] for r in range(nr)]
        mixes.append(jnp.stack([half[tuple(spot)] for spot in spots], axis=1).reshape(K, Ch))
    mix = jnp.concatenate(mixes, axis=1)

    mix, gradient, weight, scale_ratio = lax.optimization_barrier((mix, gradient, weight, scale_ratio))
    update = scale_ratio * gradient + jnp.dot(factors, mix, preferred_element_type=F32)
    new_weight = weight - 0.01 * update

    copy, last = None, nf - 1
    for r in range(nf):
        chunks = [r] if r in (0, last) else [r, r + 1]
        items = []
        for k, c in enumerate(chunks):
            direct = [it for it in gathered[c] if it[1] != nr - 1]
            relayed = [it for it in gathered[c] if it[1] == nr - 1]
            part = direct + relayed
            if r > 1 and k == 0:
                part = relayed
            if r and k == 1:
                part = direct
            items += [(x, k * nr + q, col) for x, q, col in part]
        starts = jnp.concatenate([ungray(h ^ c, nf) * nr + reps for c in chunks]).astype(jnp.int32)
        copy = place(copy, (nf * nr * R, C), starts, whole_factors, mix, nr, items)
    return (new_weight, update, new_first, new_second, copy)


def solution(mesh):
    sizes = mesh.shape
    in_specs = (
        P(("fs", "rep"), None),
        P(("fs", "rep"), "tp"),
        P(("fs", "rep"), None),
        P(("fs", "rep"), "tp"),
        P(("fs", "rep"), "tp"),
        P(("fs", "rep"), "tp"),
    )
    out_specs = (
        P(("fs", "rep"), "tp"),
        P(("fs", "rep"), "tp"),
        P(("fs", "rep"), "tp"),
        P(("fs", "rep"), "tp"),
        P(None, "tp"),
    )
    return jax.shard_map(
        functools.partial(per_device, sizes["fs"], sizes["rep"], sizes["tp"]),
        mesh=mesh,
        in_specs=in_specs,
        out_specs=out_specs,
        check_vma=False,
    )
```
